32 devices in a mesh: rep: 2 (over x), fs: 8 (over z, y), tp: 2 (over core).
Axes of the slice: x: 2, y: 2, z: 4, core: 2. Of those that a mesh axis runs over, the one named last changes fastest.
Arguments:
- tokens: bfloat16 [16384, 2048], P(('rep', 'fs', 'tp')), may hold values from -6 to 6
- pre_gain: bfloat16 [2048], replicated, may hold values from 0.099609375 to 1.8984375
- gate_weight: bfloat16 [2048, 2816], P('fs', 'tp'), may hold values from -0.125 to 0.125
- value_weight: bfloat16 [2048, 2816], P('fs', 'tp'), may hold values from -0.125 to 0.125
- down_weight: bfloat16 [2816, 2048], P('tp', 'fs'), may hold values from -0.109375 to 0.109375
- post_gain: bfloat16 [2048], replicated, may hold values from 0.099609375 to 1.8984375
Outputs:
- updated: bfloat16 [16384, 2048], P(('rep', 'fs', 'tp'))
The draws below stay inside these ranges and needn't reach their ends.
All inputs are finite; a program needn't handle non-finite values.
Results may differ from the reference program's by a relative error of at most 0.0055.
Values may be sent and summed in bfloat16 or wider, within the bound.
A program may use at most 128 MiB of HBM per device.

```python
import jax
import jax.numpy as jnp
from jax import lax

D = 2048
FF = 2816
TOK_DEV = 512
TOKENS = 16384
N_REP = 2
N_FS = 8
N_TP = 2


def block_levels(own_key, dims, cuts, low, largest):
    def one(axis_at, shards_of):
        draws = jax.random.uniform(jax.random.fold_in(jax.random.fold_in(own_key, 6), axis_at), (shards_of,), jnp.float32, low / len(cuts), largest / len(cuts))
        return jnp.repeat(jnp.exp(draws), dims[axis_at] // shards_of).reshape((-1,) + (1,) * (len(dims) - axis_at - 1))

    level = one(*cuts[0])
    for cut in cuts[1:]:
        level = level * one(*cut)
    return level


def centred(own_key, extent, scale, limit, shards=(), held_as=jnp.bfloat16):
    entries = jax.random.normal(own_key, extent, jnp.float32) * scale
    if len(shards) > 0:
        entries = block_levels(own_key, extent, shards, -0.22, 0.18) * entries
    return jnp.clip(entries, min=-limit, max=limit).astype(held_as)


def setup_inputs(seed: int = 0) -> dict:
    key_list = jax.random.split(jax.random.key(seed), 7)
    return {
        "tokens": centred(key_list[0], (TOKENS, D), 1.0, 6.0, ((0, 32),)),
        "pre_gain": jnp.clip(1.0 + 0.18 * jax.random.normal(key_list[1], (D,), jnp.float32), 0.099609375, 1.8984375).astype(jnp.bfloat16),
        "gate_weight": centred(key_list[2], (D, FF), D ** -0.5, 0.125, ((0, 8), (1, 2))),
        "value_weight": centred(key_list[3], (D, FF), D ** -0.5, 0.125, ((0, 8), (1, 2))),
        "down_weight": centred(key_list[4], (FF, D), FF ** -0.5, 0.109375, ((0, 2), (1, 8))),
        "post_gain": jnp.clip(1.0 + 0.18 * jax.random.normal(key_list[5], (D,), jnp.float32), 0.099609375, 1.8984375).astype(jnp.bfloat16),
    }


eps_norm = 1e-06

def rms_rows(values_in, gain):
    floats = values_in.astype(jnp.float32)
    scaled = floats * lax.rsqrt(lax.optimization_barrier(jnp.mean(floats * floats, -1, keepdims=True)) + eps_norm)
    return scaled * gain.astype(jnp.float32)

def reference(tokens, pre_gain, gate_weight, value_weight, down_weight, post_gain):
    group_size = TOK_DEV * N_TP
    block_width = FF // N_TP
    grouped = tokens.reshape(N_REP * N_FS, group_size, D)

    def one_group(block_rows):
        normed = rms_rows(block_rows, pre_gain).astype(jnp.bfloat16)
        gate_proj = jnp.dot(normed, gate_weight, preferred_element_type=jnp.float32)
        value_proj = jnp.dot(normed, value_weight, preferred_element_type=jnp.float32)
        hidden = (jax.nn.silu(gate_proj) * value_proj).astype(jnp.bfloat16)
        total = jnp.zeros((group_size, D), jnp.float32)
        for block_index in range(N_TP):
            lower = block_index * block_width
            partial_term = jnp.dot(hidden[:, lower:lower + block_width], down_weight[lower:lower + block_width], preferred_element_type=jnp.float32).astype(jnp.bfloat16)
            total = total + lax.optimization_barrier(partial_term).astype(jnp.float32)
        branch = total.astype(jnp.bfloat16)
        return (block_rows.astype(jnp.float32) + 0.5 * rms_rows(branch, post_gain)).astype(jnp.bfloat16)
    return lax.map(one_group, grouped).reshape(TOKENS, D)
```

```python
import functools

import jax
import jax.numpy as jnp
from jax import lax
from jax.experimental import pallas as pl
from jax.experimental.pallas import tpu as pltpu
from jax.sharding import PartitionSpec as P

eps_norm = 1e-06
MESH = pl.DeviceIdType.MESH
f32 = jnp.float32
bf16 = jnp.bfloat16


def third(rows):
    return max(rows // 3 // 16, 1) * 16


def half_of(rows):
    return (rows // 2 + 15) // 16 * 16


def when(condition, action):
    if isinstance(condition, bool):
        if condition:
            action()
    else:
        pl.when(condition)(action)


def kernel(
    n, tok_ref, pre_ref, post_ref, g_ref, v_ref, d_ref, out_ref,
    gbuf, vbuf, dbuf, nbuf, peer, gacc, vacc, hid, precv,
    send_sem, recv_sem, tok_sem, part_send, part_recv, own_sem,
):
    T, D = tok_ref.shape
    R = gbuf.shape[1]
    F = dbuf.shape[1]
    half = n // 2
    rep = lax.axis_index("rep")
    me = lax.axis_index("fs")
    core = lax.axis_index("tp")
    odd = me % 2
    pos = (1 - odd) * (me // 2) + odd * (n - 1 - me // 2)

    def fs_at(at):
        late = at // half
        return (1 - late) * 2 * at + late * (2 * (n - 1 - at) + 1)

    right = fs_at((pos + 1) % n)
    left = fs_at((pos + n - 1) % n)
    other_rep = 1 - rep
    other_core = 1 - core

    def origin(k):
        return fs_at((pos + 2 * n - 1 - k) % n)

    a, b = third(R), third(F)
    b0, c0 = half_of(b), half_of(F - 2 * b)
    chunks = (
        (gbuf, a, 0, a, 2 * a, R - 2 * a),
        (vbuf, a, 0, a, 2 * a, R - 2 * a),
        (dbuf, b, 0, b0, 2 * b, c0),
        (dbuf, b, b0, b - b0, 2 * b + c0, F - 2 * b - c0),
    )

    def part(c, k, which):
        buf, size, start, length = chunks[c][:4]
        return buf.at[k, pl.ds(pl.multiple_of(which * size + start, 16), length)]

    def common(c, k):
        return chunks[c][0].at[k, pl.ds(chunks[c][4], chunks[c][5])]

    def remote(src, dst, way, c, s, to):
        return pltpu.make_async_remote_copy(
            src_ref=src, dst_ref=dst, send_sem=send_sem.at[way, c, s], recv_sem=recv_sem.at[way, c, s],
            device_id=to, device_id_type=MESH,
        )

    def cw(s, c):
        return remote(part(c, (s + n - 1) % n, rep), part(c, s, rep), 0, c, s, {"fs": right})

    def ccw(s, c):
        return remote(common(c, n - 1 - s), common(c, n - 2 - s), 1, c, s, {"fs": left})

    def cross(s, c):
        return remote(part(c, s, rep), part(c, s, rep), 2, c, s, {"rep": other_rep})

    def cross_in(s, c):
        return remote(part(c, s, other_rep), part(c, s, other_rep), 2, c, s, {"rep": other_rep})

    def pump(s, c):
        more = s < n - 2
        cw(s, c).wait_recv()
        when(more, lambda: cw(s + 1, c).start())
        cross(s, c).start()
        ccw(s, c).wait_recv()
        when(more, lambda: ccw(s + 1, c).start())

    def tok_copy():
        return pltpu.make_async_remote_copy(
            src_ref=tok_ref, dst_ref=peer, send_sem=tok_sem.at[0], recv_sem=tok_sem.at[1],
            device_id={"tp": other_core}, device_id_type=MESH,
        )

    def part_copy(j):
        return pltpu.make_async_remote_copy(
            src_ref=nbuf.at[j, pl.ds(T, T)], dst_ref=precv.at[j], send_sem=part_send.at[j],
            recv_sem=part_recv.at[j], device_id={"tp": other_core}, device_id_type=MESH,
        )

    own = [
        pltpu.make_async_copy(src, buf.at[n - 1], own_sem.at[i])
        for i, (src, buf) in enumerate(((g_ref, gbuf), (v_ref, vbuf), (d_ref, dbuf)))
    ]
    for copy in own:
        copy.start()

    barrier = pltpu.get_barrier_semaphore()
    for to in ({"fs": right}, {"fs": left}, {"rep": other_rep}, {"tp": other_core}):
        pl.semaphore_signal(barrier, inc=1, device_id=to, device_id_type=MESH)
    pl.semaphore_wait(barrier, 4)

    for c in range(4):
        if c < 3:
            own[c].wait()
        cw(0, c).start()
        ccw(0, c).start()
    tok_copy().start()

    rows_n = 64

    def norm_rows(src, base):
        @pl.loop(0, T // rows_n)
        def _(i):
            at = pl.ds(pl.multiple_of(i * rows_n, rows_n), rows_n)
            x = src[at, :].astype(f32)
            x = x * lax.rsqrt(jnp.mean(x * x, -1, keepdims=True) + eps_norm) * pre_ref[...].astype(f32)
            x = x.astype(bf16)
            to = pl.ds(pl.multiple_of(base + i * rows_n, rows_n), rows_n)
            for j in range(n):
                nbuf[j, to, :] = x[:, j * R:(j + 1) * R]

    norm_rows(tok_ref, 0)

    @pl.loop(0, 2 * T // rows_n)
    def _(i):
        at = pl.ds(pl.multiple_of(i * rows_n, rows_n), rows_n)
        gacc[at, :] = jnp.zeros((rows_n, F), f32)
        vacc[at, :] = jnp.zeros((rows_n, F), f32)

    tok_copy().wait_recv()
    norm_rows(peer, T)

    rows_m = 256

    def up_pair(c, buf, acc, t):
        k1, k2 = t - 1, (2 * n - 2 - t) % n
        cross_in(k1, c).wait_recv()
        when(t < n - 1, lambda: cross_in(k2, c).wait_recv())
        j1, j2 = origin(k1), origin(k2)

        @pl.loop(0, 2 * T // rows_m)
        def _(i):
            at = pl.ds(pl.multiple_of(i * rows_m, rows_m), rows_m)
            acc[at, :] += jnp.dot(nbuf[j1, at, :], buf[k1], preferred_element_type=f32) + jnp.dot(
                nbuf[j2, at, :], buf[k2], preferred_element_type=f32
            )

    @pl.loop(0, n - 2)
    def _(s):
        pump(s, 0)
        pl.when(s >= half)(lambda: up_pair(0, gbuf, gacc, s))
        pump(s, 1)
        pl.when(s >= half)(lambda: up_pair(1, vbuf, vacc, s))

    pump(n - 2, 0)
    pump(n - 2, 1)

    def pump_down(u):
        if u < half:
            pump(u, 2)
            pump(u, 3)

    pump_down(0)
    up_pair(0, gbuf, gacc, n - 2)
    pump_down(1)
    up_pair(1, vbuf, vacc, n - 2)
    pump_down(2)
    up_pair(0, gbuf, gacc, n - 1)
    pump_down(3)
    up_pair(1, vbuf, vacc, n - 1)

    @pl.loop(0, 2 * T // rows_n)
    def _(i):
        at = pl.ds(pl.multiple_of(i * rows_n, rows_n), rows_n)
        gate = gacc[at, :]
        hid[at, :] = (gate / (1.0 + jnp.exp(-gate)) * vacc[at, :]).astype(bf16)

    def down(k):
        j = origin(k)

        @pl.loop(0, 2 * T // rows_m)
        def _(i):
            at = pl.ds(pl.multiple_of((i * rows_m + T) % (2 * T), rows_m), rows_m)
            nbuf[j, at, :] = jnp.dot(hid[at, :], dbuf[k], preferred_element_type=f32).astype(bf16)

        part_copy(j).start()

    def down_in(k):
        cross_in(k, 2).wait_recv()
        cross_in(k, 3).wait_recv()

    down(n - 1)

    @pl.loop(min(4, half), n - 1)
    def _(u):
        pump(u, 2)
        pump(u, 3)

        @pl.when(u >= half)
        def _():
            down_in(u - 1)
            down(u - 1)
            down_in(n - 2 - u)
            down(n - 2 - u)

    down_in(n - 2)
    down(n - 2)

    @pl.loop(0, n)
    def _(j):
        part_copy(j).wait_recv()

    rows_o = 32

    @pl.loop(0, T // rows_o)
    def _(i):
        at = pl.ds(pl.multiple_of(i * rows_o, rows_o), rows_o)
        total = jnp.zeros((rows_o, 1), f32)
        blocks = []
        for j in range(n):
            block = (nbuf[j, at, :].astype(f32) + precv[j, at, :].astype(f32)).astype(bf16)
            blocks.append(block)
            wide = block.astype(f32)
            total += jnp.sum(wide * wide, -1, keepdims=True)
        scale = lax.rsqrt(total / D + eps_norm)
        branch = jnp.concatenate(blocks, -1).astype(f32)
        updated = tok_ref[at, :].astype(f32) + 0.5 * (branch * scale * post_ref[...].astype(f32))
        out_ref[at, :] = updated.astype(bf16)

    tok_copy().wait_send()

    @pl.loop(0, n)
    def _(j):
        part_copy(j).wait_send()

    @pl.loop(0, n - 1)
    def _(s):
        for c in range(4):
            cw(s, c).wait_send()
            ccw(s, c).wait_send()
            cross(s, c).wait_send()


def shards(n, tokens, pre_gain, gate_weight, value_weight, down_weight, post_gain):
    T, D = tokens.shape
    R, F = gate_weight.shape
    vmem = pl.BlockSpec(memory_space=pltpu.VMEM)
    hbm = pl.BlockSpec(memory_space=pl.ANY)
    dma = pltpu.SemaphoreType.DMA
    return pl.pallas_call(
        functools.partial(kernel, n),
        out_shape=jax.ShapeDtypeStruct((T, D), bf16),
        in_specs=[vmem, vmem, vmem, hbm, hbm, hbm],
        out_specs=vmem,
        scratch_shapes=[
            pltpu.VMEM((n, R, F), bf16),
            pltpu.VMEM((n, R, F), bf16),
            pltpu.VMEM((n, F, R), bf16),
            pltpu.VMEM((n, 2 * T, R), bf16),
            pltpu.VMEM((T, D), bf16),
            pltpu.VMEM((2 * T, F), f32),
            pltpu.VMEM((2 * T, F), f32),
            pltpu.VMEM((2 * T, F), bf16),
            pltpu.VMEM((n, T, R), bf16),
            dma((3, 4, n - 1)),
            dma((3, 4, n - 1)),
            dma((2,)),
            dma((n,)),
            dma((n,)),
            dma((3,)),
        ],
        compiler_params=pltpu.CompilerParams(
            collective_id=0, has_side_effects=True, vmem_limit_bytes=67043328
        ),
    )(tokens, pre_gain.reshape(1, D), post_gain.reshape(1, D), gate_weight, value_weight, down_weight)


def solution(mesh):
    assert mesh.shape["rep"] == 2 and mesh.shape["tp"] == 2
    placed = (P(("rep", "fs", "tp"), None), P(), P("fs", "tp"), P("fs", "tp"), P("tp", "fs"), P())
    return jax.shard_map(
        functools.partial(shards, mesh.shape["fs"]),
        mesh=mesh, in_specs=placed, out_specs=P(("rep", "fs", "tp"), None), check_vma=False,
    )
```

```python
import functools

import jax
import jax.numpy as jnp
from jax import lax
from jax.experimental import pallas as pl
from jax.experimental.pallas import tpu as pltpu
from jax.sharding import PartitionSpec as P

eps_norm = 1e-06
MESH = pl.DeviceIdType.MESH
f32 = jnp.float32
bf16 = jnp.bfloat16


def ring_rows(R, F):
    gate = max(R // 48, 1) * 16
    value = min((R + 47) // 48 * 16, (R - 16) // 32 * 16)
    down = min(round((R - gate - value) * F / R / 16) * 16, (F - 128) // 32 * 16)
    return gate, value, down


UP_CUTS, DOWN_CUTS = 2, 2


def cut(rows, pieces):
    tiles = rows // 16
    edges = [tiles * i // pieces * 16 for i in range(pieces)] + [rows]
    return [(low, high - low) for low, high in zip(edges, edges[1:])]


def up_cuts(R, F):
    gate, value, _ = ring_rows(R, F)
    return min(UP_CUTS, gate // 16, (R - 2 * value) // 16)


def when(condition, action):
    if isinstance(condition, bool):
        if condition:
            action()
    else:
        pl.when(condition)(action)


def kernel(
    n, tok_ref, pre_ref, g_ref, v_ref, d_ref, branch_ref,
    gbuf, vbuf, dbuf, nbuf, peer, gacc, vacc, hid, precv,
    send_sem, recv_sem, tok_sem, part_send, part_recv, own_sem, branch_sem,
):
    T, D = tok_ref.shape
    R = gbuf.shape[1]
    F = dbuf.shape[1]
    half = n // 2
    rep = lax.axis_index("rep")
    me = lax.axis_index("fs")
    core = lax.axis_index("tp")
    odd = me % 2
    pos = (1 - odd) * (me // 2) + odd * (n - 1 - me // 2)

    def fs_at(at):
        late = at // half
        return (1 - late) * 2 * at + late * (2 * (n - 1 - at) + 1)

    right = fs_at((pos + 1) % n)
    left = fs_at((pos + n - 1) % n)
    other_rep = 1 - rep
    other_core = 1 - core

    def origin(k):
        return fs_at((pos + 2 * n - 1 - k) % n)

    def cuts(buf, rows, size, pieces):
        return [
            (buf, size, low, length, 2 * size + low_c, length_c)
            for (low, length), (low_c, length_c) in zip(cut(size, pieces), cut(rows - 2 * size, pieces))
        ]

    ups = up_cuts(R, F)
    sizes = ring_rows(R, F)
    chunks = cuts(gbuf, R, sizes[0], ups) + cuts(vbuf, R, sizes[1], ups) + cuts(dbuf, F, sizes[2], DOWN_CUTS)
    gate_set, value_set = range(ups), range(ups, 2 * ups)
    down_set = range(2 * ups, 2 * ups + DOWN_CUTS)

    def part(c, k, which):
        buf, size, start, length = chunks[c][:4]
        return buf.at[k, pl.ds(pl.multiple_of(which * size + start, 16), length)]

    def common(c, k):
        return chunks[c][0].at[k, pl.ds(chunks[c][4], chunks[c][5])]

    def remote(src, dst, way, c, s, to):
        return pltpu.make_async_remote_copy(
            src_ref=src, dst_ref=dst, send_sem=send_sem.at[way, c, s], recv_sem=recv_sem.at[way, c, s],
            device_id=to, device_id_type=MESH,
        )

    def cw(s, c):
        return remote(part(c, (s + n - 1) % n, rep), part(c, s, rep), 0, c, s, {"fs": right})

    def ccw(s, c):
        return remote(common(c, n - 1 - s), common(c, n - 2 - s), 1, c, s, {"fs": left})

    def cross(s, c):
        return remote(part(c, s, rep), part(c, s, rep), 2, c, s, {"rep": other_rep})

    def cross_in(s, c):
        return remote(part(c, s, other_rep), part(c, s, other_rep), 2, c, s, {"rep": other_rep})

    def pump(s, c):
        more = s < n - 2
        cw(s, c).wait_recv()
        when(more, lambda: cw(s + 1, c).start())
        cross(s, c).start()
        ccw(s, c).wait_recv()
        when(more, lambda: ccw(s + 1, c).start())

    def tok_copy():
        return pltpu.make_async_remote_copy(
            src_ref=tok_ref, dst_ref=peer, send_sem=tok_sem.at[0], recv_sem=tok_sem.at[1],
            device_id={"tp": other_core}, device_id_type=MESH,
        )

    def part_copy(j):
        return pltpu.make_async_remote_copy(
            src_ref=nbuf.at[j, pl.ds(T, T)], dst_ref=precv.at[j], send_sem=part_send.at[j],
            recv_sem=part_recv.at[j], device_id={"tp": other_core}, device_id_type=MESH,
        )

    own = [
        pltpu.make_async_copy(src, buf.at[n - 1], own_sem.at[i])
        for i, (src, buf) in enumerate(((g_ref, gbuf), (v_ref, vbuf), (d_ref, dbuf)))
    ]
    for copy in own:
        copy.start()

    barrier = pltpu.get_barrier_semaphore()
    for to in ({"fs": right}, {"fs": left}, {"rep": other_rep}, {"tp": other_core}):
        pl.semaphore_signal(barrier, inc=1, device_id=to, device_id_type=MESH)
    pl.semaphore_wait(barrier, 4)

    for copy, owned in zip(own, (gate_set, value_set, down_set)):
        copy.wait()
        for c in owned:
            cw(0, c).start()
            ccw(0, c).start()
    tok_copy().start()

    rows_n = 64

    def norm_rows(src, base):
        @pl.loop(0, T // rows_n)
        def _(i):
            at = pl.ds(pl.multiple_of(i * rows_n, rows_n), rows_n)
            x = src[at, :].astype(f32)
            x = x * lax.rsqrt(jnp.mean(x * x, -1, keepdims=True) + eps_norm) * pre_ref[...].astype(f32)[None, :]
            x = x.astype(bf16)
            to = pl.ds(pl.multiple_of(base + i * rows_n, rows_n), rows_n)
            for j in range(n):
                nbuf[j, to, :] = x[:, j * R:(j + 1) * R]

    norm_rows(tok_ref, 0)

    @pl.loop(0, 2 * T // rows_n)
    def _(i):
        at = pl.ds(pl.multiple_of(i * rows_n, rows_n), rows_n)
        gacc[at, :] = jnp.zeros((rows_n, F), f32)
        vacc[at, :] = jnp.zeros((rows_n, F), f32)

    tok_copy().wait_recv()
    norm_rows(peer, T)

    rows_m = 256

    tiles_m = 2 * T // rows_m

    def up_pair(owned, t, piece, pieces):
        buf, acc = (gbuf, gacc) if owned is gate_set else (vbuf, vacc)
        k1, k2 = t - 1, (2 * n - 2 - t) % n
        if piece == 0:
            for c in owned:
                cross_in(k1, c).wait_recv()
                when(t < n - 1, lambda: cross_in(k2, c).wait_recv())
        j1, j2 = origin(k1), origin(k2)

        @pl.loop(tiles_m * piece // pieces, tiles_m * (piece + 1) // pieces)
        def _(i):
            at = pl.ds(pl.multiple_of(i * rows_m, rows_m), rows_m)
            acc[at, :] += jnp.dot(nbuf[j1, at, :], buf[k1], preferred_element_type=f32) + jnp.dot(
                nbuf[j2, at, :], buf[k2], preferred_element_type=f32
            )

    @pl.loop(0, n - 1)
    def _(s):
        for i, c in enumerate(gate_set):
            pump(s, c)
            pl.when(s > half)(lambda: up_pair(value_set, s - 1, i, ups))
        for i, c in enumerate(value_set):
            pump(s, c)
            pl.when(s >= half)(lambda: up_pair(gate_set, s, i, ups))

    def pump_down(u):
        for c in down_set:
            pump(u, c)

    early = min(4, half)
    pump_down(0)
    up_pair(value_set, n - 2, 0, 1)
    if early > 1:
        pump_down(1)
    up_pair(gate_set, n - 1, 0, 1)
    if early > 2:
        pump_down(2)
    up_pair(value_set, n - 1, 0, 1)
    if early > 3:
        pump_down(3)

    @pl.loop(0, 2 * T // rows_n)
    def _(i):
        at = pl.ds(pl.multiple_of(i * rows_n, rows_n), rows_n)
        gate = gacc[at, :]
        hid[at, :] = (gate / (1.0 + jnp.exp(-gate)) * vacc[at, :]).astype(bf16)

    def down(k):
        j = origin(k)

        @pl.loop(0, 2 * T // rows_m)
        def _(i):
            at = pl.ds(pl.multiple_of((i * rows_m + T) % (2 * T), rows_m), rows_m)
            nbuf[j, at, :] = jnp.dot(hid[at, :], dbuf[k], preferred_element_type=f32).astype(bf16)

        part_copy(j).start()

    def down_in(k):
        for c in down_set:
            cross_in(k, c).wait_recv()

    down(n - 1)

    @pl.loop(early, n - 1)
    def _(u):
        pump_down(u)

        @pl.when(u >= half)
        def _():
            down_in(u - 1)
            down(u - 1)
            down_in(n - 2 - u)
            down(n - 2 - u)

    down_in(n - 2)
    down(n - 2)

    def finish(k):
        j = origin(k)
        part_copy(j).wait_recv()

        @pl.loop(0, T // rows_n)
        def _(i):
            at = pl.ds(pl.multiple_of(i * rows_n, rows_n), rows_n)
            nbuf[j, at, :] = (nbuf[j, at, :].astype(f32) + precv[j, at, :].astype(f32)).astype(bf16)

        branch_copy(j).start()

    def branch_copy(j):
        return pltpu.make_async_copy(nbuf.at[j, pl.ds(0, T)], branch_ref.at[j], branch_sem.at[j])

    finish(n - 1)

    @pl.loop(0, n - 1)
    def _(k):
        finish(k)

    @pl.loop(0, n)
    def _(j):
        branch_copy(j).wait()

    tok_copy().wait_send()

    @pl.loop(0, n)
    def _(j):
        part_copy(j).wait_send()

    @pl.loop(0, n - 1)
    def _(s):
        for c in range(len(chunks)):
            cw(s, c).wait_send()
            ccw(s, c).wait_send()
            cross(s, c).wait_send()


def add_normed(branch_ref, tok_ref, post_ref, out_ref):
    n, rows, R = branch_ref.shape
    D = tok_ref.shape[1]
    total = jnp.zeros((rows, 1), f32)
    for j in range(n):
        wide = branch_ref[j].astype(f32)
        total += jnp.sum(wide * wide, -1, keepdims=True)
    scale = 0.5 * lax.rsqrt(total / D + eps_norm)
    branch = jnp.concatenate([branch_ref[j] for j in range(n)], -1).astype(f32)
    updated = tok_ref[...].astype(f32) + branch * scale * post_ref[...].astype(f32)[None, :]
    out_ref[...] = updated.astype(bf16)


def shards(n, tokens, pre_gain, gate_weight, value_weight, down_weight, post_gain):
    T, D = tokens.shape
    R, F = gate_weight.shape
    vmem = pl.BlockSpec(memory_space=pltpu.VMEM)
    hbm = pl.BlockSpec(memory_space=pl.ANY)
    dma = pltpu.SemaphoreType.DMA
    branch = pl.pallas_call(
        functools.partial(kernel, n),
        out_shape=jax.ShapeDtypeStruct((n, T, R), bf16),
        in_specs=[vmem, vmem, hbm, hbm, hbm],
        out_specs=hbm,
        scratch_shapes=[
            pltpu.VMEM((n, R, F), bf16),
            pltpu.VMEM((n, R, F), bf16),
            pltpu.VMEM((n, F, R), bf16),
            pltpu.VMEM((n, 2 * T, R), bf16),
            pltpu.VMEM((T, D), bf16),
            pltpu.VMEM((2 * T, F), f32),
            pltpu.VMEM((2 * T, F), f32),
            pltpu.VMEM((2 * T, F), bf16),
            pltpu.VMEM((n, T, R), bf16),
            dma((3, 2 * up_cuts(R, F) + DOWN_CUTS, n - 1)),
            dma((3, 2 * up_cuts(R, F) + DOWN_CUTS, n - 1)),
            dma((2,)),
            dma((n,)),
            dma((n,)),
            dma((3,)),
            dma((n,)),
        ],
        compiler_params=pltpu.CompilerParams(
            collective_id=0, has_side_effects=True, vmem_limit_bytes=67043328
        ),
    )(tokens, pre_gain, gate_weight, value_weight, down_weight)
    rows = 128
    return pl.pallas_call(
        add_normed,
        grid=(T // rows,),
        out_shape=jax.ShapeDtypeStruct((T, D), bf16),
        in_specs=[
            pl.BlockSpec((n, rows, R), lambda i: (0, i, 0)),
            pl.BlockSpec((rows, D), lambda i: (i, 0)),
            pl.BlockSpec((D,), lambda i: (0,)),
        ],
        out_specs=pl.BlockSpec((rows, D), lambda i: (i, 0)),
    )(branch, tokens, post_gain)


def solution(mesh):
    assert mesh.shape["rep"] == 2 and mesh.shape["tp"] == 2
    placed = (P(("rep", "fs", "tp"), None), P(), P("fs", "tp"), P("fs", "tp"), P("tp", "fs"), P())
    return jax.shard_map(
        functools.partial(shards, mesh.shape["fs"]),
        mesh=mesh, in_specs=placed, out_specs=P(("rep", "fs", "tp"), None), check_vma=False,
    )
```
